512 devices in a mesh: ra: 16 (over y, x), cb: 32 (over z, core).
Axes of the slice: x: 4, y: 4, z: 16, core: 2. Of those that a mesh axis runs over, the one named last changes fastest.
Arguments:
- tokens: bfloat16 [256, 4096], P(None, 'ra'), may hold values from -20 to 20, as said below
- norm_gain: float32 [2, 4096], P(None, 'ra'), may hold values from 0.1 to 1.9
- gate_weight: bfloat16 [2, 4096, 11008], P(None, 'ra', 'cb'), may hold values from -0.09375 to 0.09375
- value_weight: bfloat16 [2, 4096, 11008], P(None, 'ra', 'cb'), may hold values from -0.09375 to 0.09375
- gate_taps: float32 [2, 3, 11008], P(None, None, 'cb'), may hold values from -3.5 to 3.5
- value_taps: float32 [2, 3, 11008], P(None, None, 'cb'), may hold values from -3.5 to 3.5
- down_weight: bfloat16 [2, 11008, 4096], P(None, 'cb', 'ra'), may hold values from -0.0546875 to 0.0546875
Outputs:
- mixed: bfloat16 [256, 4096], P(None, 'ra')
The draws below stay inside these ranges and needn't reach their ends.
Inputs may be any that keep to these rules, and one draw needn't show every extreme that they name: tokens have features drawn around zero with a scale that varies by blocks of features between about 0.3 and 3.3.
All inputs are finite; a program needn't handle non-finite values.
Results may differ from the reference program's by a relative error of at most 0.0075.
Values may be sent and summed in bfloat16 or wider, within the bound.
A program may use at most 128 MiB of HBM per device.

```python
import jax
import jax.numpy as jnp
from jax import lax

D = 4096
FF = 11008
KERNEL = 3
LAYERS = 2
TOKENS = 256


def draw_tokens(key, part):
    base_key, scale_key = jax.random.split(jax.random.fold_in(key, 11))
    block_scales = jnp.exp(jax.random.uniform(scale_key, (64,), jnp.float32, -1.2, 1.2))
    column_scales = jnp.repeat(block_scales, D // 64)
    base = jnp.clip(jax.random.normal(base_key, (TOKENS, D), jnp.float32), -6.0, 6.0)
    return (base * column_scales[None, :]).astype(jnp.bfloat16)


def block_levels(stream_key, shape, pieces, least, top_value):
    factor_of = 1.0
    for position, blocks in pieces:
        draws = jax.random.uniform(jax.random.fold_in(jax.random.fold_in(stream_key, 6), position), (blocks,), jnp.float32, least / len(pieces), top_value / len(pieces))
        factor_of = factor_of * jnp.repeat(jnp.exp(draws), shape[position] // blocks).reshape((-1,) + (1,) * (len(shape) - 1 - position))
    return factor_of


def bell_draw(stream_key, dims, spread, most, shards=(), held_as=jnp.bfloat16):
    drawn = spread * jax.random.normal(stream_key, dims, jnp.float32)
    if shards:
        drawn = drawn * block_levels(stream_key, dims, shards, -0.22, 0.18)
    return jnp.clip(drawn, -most, most).astype(held_as)


def setup_inputs(seed: int = 0) -> dict:
    keys = jax.random.split(jax.random.key(seed), 8)
    return {
        "tokens": draw_tokens(jax.random.fold_in(keys[7], 71), 0),
        "norm_gain": jnp.clip(1.0 + 0.18 * jax.random.normal(keys[1], (LAYERS, D), jnp.float32), 0.1, 1.9),
        "gate_weight": bell_draw(keys[2], (LAYERS, D, FF), D ** -0.5, 0.09375, ((1, 16), (2, 32))),
        "value_weight": bell_draw(keys[3], (LAYERS, D, FF), D ** -0.5, 0.09375, ((1, 16), (2, 32))),
        "gate_taps": bell_draw(keys[4], (LAYERS, KERNEL, FF), KERNEL ** -0.5, 3.5, ((2, 32),), jnp.float32),
        "value_taps": bell_draw(keys[5], (LAYERS, KERNEL, FF), KERNEL ** -0.5, 3.5, ((2, 32),), jnp.float32),
        "down_weight": bell_draw(keys[6], (LAYERS, FF, D), FF ** -0.5, 0.0546875, ((1, 32), (2, 16))),
    }


epsilon = 1e-06

def causal_conv(signal, kernel_taps):
    length = signal.shape[0]
    width = kernel_taps.shape[0]
    padded = jnp.concatenate([jnp.zeros((width - 1, signal.shape[1]), jnp.float32), signal], axis=0)
    result = jnp.zeros(signal.shape, jnp.float32)
    for offset in range(width):
        result = result + kernel_taps[offset] * padded[offset:offset + length]
    return result

def reference(tokens, norm_gain, gate_weight, value_weight, gate_taps, value_taps, down_weight):
    stream = tokens
    for layer_index in range(LAYERS):
        current = stream.astype(jnp.float32)
        inverse_rms = lax.rsqrt(lax.optimization_barrier(jnp.sum(current * current, axis=1, keepdims=True)) / D + epsilon)
        scaled = (current * norm_gain[layer_index]).astype(jnp.bfloat16)
        gate_lin = jnp.dot(scaled, gate_weight[layer_index], preferred_element_type=jnp.float32) * inverse_rms
        value_lin = jnp.dot(scaled, value_weight[layer_index], preferred_element_type=jnp.float32) * inverse_rms
        gate_conv = causal_conv(gate_lin, gate_taps[layer_index])
        value_conv = causal_conv(value_lin, value_taps[layer_index])
        hidden = (jax.nn.silu(gate_conv) * value_conv).astype(jnp.bfloat16)
        branch = jnp.dot(hidden, down_weight[layer_index], preferred_element_type=jnp.float32)
        stream = (0.5 * current + branch).astype(jnp.bfloat16)
    return stream
```

```python
import functools

import jax
import jax.numpy as jnp
from jax import lax
from jax.experimental import pallas as pl
from jax.experimental.pallas import tpu as pltpu
from jax.sharding import PartitionSpec as P

MESH = pl.DeviceIdType.MESH
F32, BF16 = jnp.float32, jnp.bfloat16
EPS = 1e-06
ROWS = 16
LANE = 128
STOP = 99


def round_up(n, m):
    return (n + m - 1) // m * m


def kernel(ny, nx, nz, width, tok, gain, gw, vw, gt, vt, dw, out, gain_v, gw_v, vw_v, gt_v, vt_v, dw_v,
           wcat, dcat, tcat, xs, up_send, halo_send, up_recv, halo_recv, conv_buf, hid_all, branch_own, br_send,
           pair_recv, z_send, z_recv, load_sem, send_sem, recv_sem):
    layers, feats, units = gw_v.shape
    pad = round_up(units, LANE)
    tail = pad - LANE
    nr = ny * nx
    tokens = nr * ROWS
    me = lax.axis_index("ra")
    my = lax.axis_index("cb")
    y, x = me // nx, lax.rem(me, nx)
    z, c = my // 2, lax.rem(my, 2)
    other = 1 - c

    def ra_peer(dy, dx):
        return lax.rem(y + dy, ny) * nx + lax.rem(x + dx, nx)

    loads = []
    pairs = [(tok.at[:, :LANE], xs.at[0, 0]), (tok.at[:, LANE:], xs.at[0, 1]), (gain, gain_v), (gw, gw_v), (vw, vw_v), (gt, gt_v), (vt, vt_v), (dw, dw_v)]
    for i, (a, b) in enumerate(pairs):
        copy = pltpu.make_async_copy(a, b, load_sem.at[i])
        copy.start()
        loads.append(copy)

    barrier = pltpu.get_barrier_semaphore()

    def greet_ra(d, carry):
        pl.semaphore_signal(barrier, inc=1, device_id=(ra_peer(d // nx, lax.rem(d, nx)), my), device_id_type=MESH)
        return carry

    def greet_cb(d, carry):
        pl.semaphore_signal(barrier, inc=1, device_id=(me, lax.rem(z + d, nz) * 2 + c), device_id_type=MESH)
        return carry

    lax.fori_loop(1, nz, greet_cb, 0)
    lax.fori_loop(1, nr, greet_ra, 0)
    pl.semaphore_signal(barrier, inc=1, device_id=(me, z * 2 + other), device_id_type=MESH)

    wcat[...] = jnp.zeros_like(wcat)
    dcat[...] = jnp.zeros_like(dcat)
    tcat[...] = jnp.zeros_like(tcat)
    for copy in loads:
        copy.wait()
    for l in range(layers):
        wcat[l, :, :units] = gw_v[l]
        wcat[l, :, pad:pad + units] = vw_v[l]
        dcat[l, :units, :] = dw_v[l]
        tcat[l, :, :units] = gt_v[l]
        tcat[l, :, pad:pad + units] = vt_v[l]

    ra_order = sorted(range(1, nr), key=lambda d: -(min(d // nx, ny - d // nx) + min(d % nx, nx - d % nx)))
    z_order = sorted(range(1, nz), key=lambda d: -min(d, nz - d))
    sends = []

    def wait_all(ref, sem):
        pltpu.make_async_copy(ref, ref, sem).wait()

    stage = 0
    for l in range(layers):
        if STOP < 6 * l + 1:
            break
        cur = jnp.concatenate([xs[l, 0], xs[l, 1]], axis=1).astype(F32)
        ssq = jnp.sum(cur * cur, axis=1, keepdims=True)
        high = ssq.astype(BF16).astype(F32)
        low = ssq - high
        scaled = (cur * gain_v[l:l + 1, :]).astype(BF16)
        up = jnp.dot(scaled, wcat[l], preferred_element_type=F32)
        lane = lax.broadcasted_iota(jnp.int32, (tokens, LANE), 1) + tail
        spare = jnp.where(lane == units, high, jnp.where(lane == units + 1, low, up[:, tail:pad]))
        up_send[l, :, :tail] = up[:, :tail].astype(BF16)
        up_send[l, :, tail:pad] = spare.astype(BF16)
        up_send[l, :, pad:] = up[:, pad:].astype(BF16)
        for t in range(nr):
            halo_send[l, t] = up_send[l, t * ROWS:(t + 1) * ROWS, :].astype(F32)[ROWS - 2:, :].astype(BF16)
        if l == 0:
            pl.semaphore_wait(barrier, nr + nz - 1)
        for d in ra_order:
            peer = ra_peer(d // nx, d % nx)
            pltpu.make_async_remote_copy(
                src_ref=up_send.at[l, pl.ds(pl.multiple_of(peer * ROWS, ROWS), ROWS)], dst_ref=up_recv.at[l, d - 1],
                send_sem=send_sem.at[l, 0], recv_sem=recv_sem.at[l, 0], device_id=(peer, my), device_id_type=MESH).start()
            before = lax.rem(peer + nr - 1, nr)
            pltpu.make_async_remote_copy(
                src_ref=halo_send.at[l, before], dst_ref=halo_recv.at[l, d - 1],
                send_sem=send_sem.at[l, 1], recv_sem=recv_sem.at[l, 1], device_id=(peer, my), device_id_type=MESH).start()
        sends.append((up_recv.at[l], send_sem.at[l, 0]))
        sends.append((halo_recv.at[l], send_sem.at[l, 1]))
        total = up_send[l, pl.ds(pl.multiple_of(me * ROWS, ROWS), ROWS), :].astype(F32)
        edge = halo_send[l, lax.rem(me + nr - 1, nr)].astype(F32)
        wait_all(up_recv.at[l], recv_sem.at[l, 0])
        wait_all(halo_recv.at[l], recv_sem.at[l, 1])
        if STOP < 6 * l + 2:
            break
        for d in range(nr - 1):
            total = total + up_recv[l, d].astype(F32)
            edge = edge + halo_recv[l, d].astype(F32)

        def normed(block):
            spot = lax.broadcasted_iota(jnp.int32, (block.shape[0], LANE), 1) + tail
            held = jnp.logical_or(spot == units, spot == units + 1)
            meansq = jnp.sum(jnp.where(held, block[:, tail:pad], 0.0), axis=1, keepdims=True) / width
            return block * lax.rsqrt(meansq + EPS)

        conv_buf[8:8 + ROWS, :] = normed(total)
        conv_buf[6:8, :] = jnp.where(me > 0, normed(edge), 0.0)
        conv = tcat[l, 0:1, :] * conv_buf[6:6 + ROWS, :]
        conv = conv + tcat[l, 1:2, :] * conv_buf[7:7 + ROWS, :]
        conv = conv + tcat[l, 2:3, :] * conv_buf[8:8 + ROWS, :]
        gate, value = conv[:, :pad], conv[:, pad:]
        hidden = gate / (1.0 + jnp.exp(-gate)) * value
        column = lax.broadcasted_iota(jnp.int32, (ROWS, pad), 1)
        hid_all[l, me] = jnp.where(column < units, hidden, 0.0).astype(BF16)
        for d in ra_order:
            peer = ra_peer(d // nx, d % nx)
            pltpu.make_async_remote_copy(
                src_ref=hid_all.at[l, me], dst_ref=hid_all.at[l, me],
                send_sem=send_sem.at[l, 2], recv_sem=recv_sem.at[l, 2], device_id=(peer, my), device_id_type=MESH).start()
        others = hid_all.at[l, pl.ds(0, nr - 1)]
        sends.append((others, send_sem.at[l, 2]))
        wait_all(others, recv_sem.at[l, 2])
        if STOP < 6 * l + 3:
            break
        hid = hid_all[l].reshape(tokens, pad)
        part = jnp.dot(hid, dcat[l], preferred_element_type=F32)
        for h in range(2):
            piece = part[:, h * LANE:(h + 1) * LANE]
            branch_own[h] = piece
            br_send[l, h] = piece.astype(BF16)
        pair = pltpu.make_async_remote_copy(
            src_ref=br_send.at[l, other], dst_ref=pair_recv.at[l],
            send_sem=send_sem.at[l, 3], recv_sem=recv_sem.at[l, 3], device_id=(me, z * 2 + other), device_id_type=MESH)
        pair.start()
        sends.append((pair_recv.at[l], send_sem.at[l, 3]))
        pair.wait_recv()
        if STOP < 6 * l + 4:
            break
        z_send[l] = (branch_own[c] + pair_recv[l].astype(F32)).astype(BF16)
        for d in z_order:
            to = lax.rem(z + d, nz)
            pltpu.make_async_remote_copy(
                src_ref=z_send.at[l, pl.ds(pl.multiple_of(to * ROWS, ROWS), ROWS)], dst_ref=z_recv.at[l, d - 1],
                send_sem=send_sem.at[l, 4], recv_sem=recv_sem.at[l, 4], device_id=(me, to * 2 + c), device_id_type=MESH).start()
        sends.append((z_recv.at[l], send_sem.at[l, 4]))
        mine = pl.ds(pl.multiple_of(z * ROWS, ROWS), ROWS)
        branch = z_send[l, mine, :].astype(F32)
        wait_all(z_recv.at[l], recv_sem.at[l, 4])
        if STOP < 6 * l + 5:
            break
        for d in range(nz - 1):
            branch = branch + z_recv[l, d].astype(F32)
        xs[l + 1, c, mine, :] = (0.5 * xs[l, c, mine, :].astype(F32) + branch).astype(BF16)
        for d in z_order:
            to = lax.rem(z + d, nz)
            pltpu.make_async_remote_copy(
                src_ref=xs.at[l + 1, c, mine], dst_ref=xs.at[l + 1, c, mine],
                send_sem=send_sem.at[l, 5], recv_sem=recv_sem.at[l, 5], device_id=(me, to * 2 + c), device_id_type=MESH).start()
        sends.append((z_recv.at[l], send_sem.at[l, 5]))
        wait_all(z_recv.at[l], recv_sem.at[l, 5])
        if STOP < 6 * l + 6:
            break
        swap = pltpu.make_async_remote_copy(
            src_ref=xs.at[l + 1, c], dst_ref=xs.at[l + 1, c],
            send_sem=send_sem.at[l, 6], recv_sem=recv_sem.at[l, 6], device_id=(me, z * 2 + other), device_id_type=MESH)
        swap.start()
        sends.append((pair_recv.at[l], send_sem.at[l, 6]))
        swap.wait_recv()

    if STOP == 0:
        pl.semaphore_wait(barrier, nr + nz - 1)
    stores = []
    for h in range(2):
        store = pltpu.make_async_copy(xs.at[layers if STOP > 90 else 0, h], out.at[:, h * LANE:(h + 1) * LANE], load_sem.at[h])
        store.start()
        stores.append(store)
    for ref, sem in sends:
        wait_all(ref, sem)
    for store in stores:
        store.wait()


def run(ny, nx, nz, width, tokens, norm_gain, gate_weight, value_weight, gate_taps, value_taps, down_weight):
    layers, feats, units = gate_weight.shape
    count = tokens.shape[0]
    pad = round_up(units, LANE)
    nr = ny * nx
    taps = gate_taps.shape[1]
    scratch = [
        pltpu.VMEM((layers, feats), F32),
        pltpu.VMEM((layers, feats, units), BF16),
        pltpu.VMEM((layers, feats, units), BF16),
        pltpu.VMEM((layers, taps, units), F32),
        pltpu.VMEM((layers, taps, units), F32),
        pltpu.VMEM((layers, units, feats), BF16),
        pltpu.VMEM((layers, feats, 2 * pad), BF16),
        pltpu.VMEM((layers, pad, feats), BF16),
        pltpu.VMEM((layers, taps, 2 * pad), F32),
        pltpu.VMEM((layers + 1, 2, count, LANE), BF16),
        pltpu.VMEM((layers, count, 2 * pad), BF16),
        pltpu.VMEM((layers, nr, 2, 2 * pad), BF16),
        pltpu.VMEM((layers, nr - 1, ROWS, 2 * pad), BF16),
        pltpu.VMEM((layers, nr - 1, 2, 2 * pad), BF16),
        pltpu.VMEM((8 + ROWS, 2 * pad), F32),
        pltpu.VMEM((layers, nr, ROWS, pad), BF16),
        pltpu.VMEM((2, count, LANE), F32),
        pltpu.VMEM((layers, 2, count, LANE), BF16),
        pltpu.VMEM((layers, count, LANE), BF16),
        pltpu.VMEM((layers, count, LANE), BF16),
        pltpu.VMEM((layers, nz - 1, ROWS, LANE), BF16),
        pltpu.SemaphoreType.DMA((8,)),
        pltpu.SemaphoreType.DMA((layers, 7)),
        pltpu.SemaphoreType.DMA((layers, 7)),
    ]
    return pl.pallas_call(
        functools.partial(kernel, ny, nx, nz, width),
        out_shape=jax.ShapeDtypeStruct(tokens.shape, tokens.dtype),
        in_specs=[pl.BlockSpec(memory_space=pl.ANY)] * 7,
        out_specs=pl.BlockSpec(memory_space=pl.ANY),
        scratch_shapes=scratch,
        compiler_params=pltpu.CompilerParams(collective_id=0, has_side_effects=True, vmem_limit_bytes=40 * 1024 * 1024),
    )(tokens, norm_gain, gate_weight, value_weight, gate_taps, value_taps, down_weight)


def solution(mesh):
    nr, nz = mesh.shape["ra"], mesh.shape["cb"] // 2
    side = int(round(nr ** 0.5))

    def body(tokens, *rest):
        return run(side, side, nz, tokens.shape[1] * nr, tokens, *rest)

    placed = (P(None, "ra"), P(None, "ra"), P(None, "ra", "cb"), P(None, "ra", "cb"), P(None, None, "cb"), P(None, None, "cb"), P(None, "cb", "ra"))
    return jax.shard_map(body, mesh=mesh, in_specs=placed, out_specs=P(None, "ra"), check_vma=False)
```
